32 devices in a mesh: grp: 2 (over x), sp: 4 (over z), tp: 4 (over y, core).
Axes of the slice: x: 2, y: 2, z: 4, core: 2. Of those that a mesh axis runs over, the one named last changes fastest.
Arguments:
- tokens: bfloat16 [1792, 4096], P(('grp', 'sp'), 'tp'), parts along dimension 0, may hold values from -130 to 130
- rms_gain: float32 [2, 4096], replicated, may hold values from 0.1 to 1.9
- w_value: bfloat16 [2, 4096, 2048], P(None, 'sp', 'tp'), may hold values from -0.09375 to 0.09375
- w_gate: bfloat16 [2, 4096, 2048], P(None, 'sp', 'tp'), may hold values from -0.09375 to 0.09375
- taps: float32 [2, 31, 2048], P(None, None, 'tp'), may hold values from -8 to 8
- ln_gain: float32 [2, 2048], P(None, 'tp'), may hold values from 0.1 to 1.9
- ln_bias: float32 [2, 2048], P(None, 'tp'), may hold values from -3 to 3
- w_out: bfloat16 [2, 2048, 4096], P(None, 'sp', 'tp'), may hold values from -0.125 to 0.125
Outputs:
- result: bfloat16 [1792, 4096], P(('grp', 'sp'), 'tp'), parts along dimension 0
The draws below stay inside these ranges and needn't reach their ends.
There are 2 independent parts, one for each index of `grp`. The reference program is written for one: setup_inputs(seed, part) draws one part's arguments, and reference() takes and returns one part's arrays. A program takes and returns all parts, laid end to end along the dimension named above; an argument that names none is the same for every part. Nothing has to cross between parts.
All inputs are finite; a program needn't handle non-finite values.
Results may differ from the reference program's by a relative error of at most 0.009.
Values may be sent and summed in bfloat16 or wider, within the bound.
No kernel may reach another device: no remote copies, remote signals or barrier semaphores. Data moves between devices by JAX's collectives and lax.ppermute only.
A program may use at most 64 MiB of HBM per device.

```python
import jax
import jax.numpy as jnp
from jax import lax

D = 4096
CH = 2048
WIDTH = 31
LAYERS = 2
TOKENS = 896


def draw_tokens(key, part):
    keys = jax.random.split(jax.random.fold_in(key, 11), 3)
    column = jnp.arange(D, dtype=jnp.float32) / D
    col_scale = jnp.exp(jnp.log(4.0) * column + jax.random.uniform(keys[1], (D,), jnp.float32, -0.4, 0.4))
    row_scale = jnp.exp(jax.random.uniform(keys[2], (TOKENS, 1), jnp.float32, jnp.log(0.5), jnp.log(5.0)))
    base = jax.random.truncated_normal(keys[0], -4.0, 4.0, (TOKENS, D), jnp.float32)
    return (base * col_scale[None, :] * row_scale).astype(jnp.bfloat16)


def draw_taps(key, part):
    keys = jax.random.split(jax.random.fold_in(key, 23), 2)
    channel = jnp.arange(CH, dtype=jnp.float32) / CH
    scale = jnp.exp(jnp.log(10.0) * channel[None, None, :] + jax.random.uniform(keys[1], (LAYERS, 1, CH), jnp.float32, -0.3, 0.3)) / jnp.sqrt(1.0 * WIDTH)
    base = jax.random.truncated_normal(keys[0], -3.0, 3.0, (LAYERS, WIDTH, CH), jnp.float32)
    return base * scale


def level_of(key, shape, cuts, least, top_value):
    def one(dim, parts):
        draws = jax.random.uniform(jax.random.fold_in(jax.random.fold_in(key, 6), dim), (parts,), jnp.float32, least / len(cuts), top_value / len(cuts))
        return jnp.repeat(jnp.exp(draws), shape[dim] // parts).reshape((-1,) + (1,) * (len(shape) - dim - 1))

    loudness = one(*cuts[0])
    for cut in cuts[1:]:
        loudness = loudness * one(*cut)
    return loudness


def scatter_about(own_key, shape, width, reach, shards=(), kind=jnp.bfloat16):
    array = width * jax.random.normal(own_key, shape, jnp.float32)
    if shards:
        array = array * level_of(own_key, shape, shards, -0.22, 0.18)
    return jnp.clip(array, -reach, reach).astype(kind)


def setup_inputs(seed: int = 0, part: int = 0) -> dict:
    arg_keys = jax.random.split(jax.random.key(seed), 9)
    part_keys = jax.random.split(jax.random.fold_in(arg_keys[8], part), 9)
    tokens = draw_tokens(jax.random.fold_in(jax.random.fold_in(arg_keys[8], part), 71), part)
    rms_gain = jnp.clip(1.0 + 0.18 * jax.random.normal(arg_keys[1], (LAYERS, D), jnp.float32), 0.1, 1.9)
    w_value = scatter_about(arg_keys[2], (LAYERS, D, CH), D ** -0.5, 0.09375, ((1, 4), (2, 4)))
    w_gate = scatter_about(arg_keys[3], (LAYERS, D, CH), D ** -0.5, 0.09375, ((1, 4), (2, 4)))
    taps = draw_taps(jax.random.fold_in(arg_keys[8], 71), part)
    ln_gain = jnp.clip(1.0 + 0.18 * jax.random.normal(arg_keys[5], (LAYERS, CH), jnp.float32), 0.1, 1.9)
    ln_bias = scatter_about(arg_keys[6], (LAYERS, CH), 0.5, 3.0, ((1, 4),), jnp.float32)
    w_out = scatter_about(arg_keys[7], (LAYERS, CH, D), CH ** -0.5, 0.125, ((1, 4), (2, 4)))
    return dict(tokens=tokens, rms_gain=rms_gain, w_value=w_value, w_gate=w_gate, taps=taps, ln_gain=ln_gain, ln_bias=ln_bias, w_out=w_out)


def reference(tokens, rms_gain, w_value, w_gate, taps, ln_gain, ln_bias, w_out):
    hidden = tokens
    for layer in range(LAYERS):
        wide = hidden.astype(jnp.float32)
        normed = (wide * lax.rsqrt(lax.optimization_barrier(jnp.mean(wide * wide, axis=1, keepdims=True)) + 1e-06) * rms_gain[layer]).astype(jnp.bfloat16)
        value = jnp.dot(normed, w_value[layer], preferred_element_type=jnp.float32)
        gate = jnp.dot(normed, w_gate[layer], preferred_element_type=jnp.float32)
        glu = (value * jax.nn.sigmoid(gate)).astype(jnp.bfloat16)
        padded = jnp.concatenate([jnp.zeros((WIDTH - 1, CH), jnp.bfloat16), glu], axis=0).astype(jnp.float32)
        conv = jnp.zeros((TOKENS, CH), jnp.float32)
        for k in range(WIDTH):
            conv = conv + taps[layer, k][None, :] * padded[k:k + TOKENS]
        mean = lax.optimization_barrier(jnp.mean(conv, axis=1, keepdims=True))
        var = lax.optimization_barrier(jnp.mean(conv * conv, axis=1, keepdims=True)) - mean * mean
        normed_conv = (conv - mean) * lax.rsqrt(var + 1e-05) * ln_gain[layer] + ln_bias[layer]
        act = jax.nn.silu(normed_conv).astype(jnp.bfloat16)
        branch = jnp.dot(act, w_out[layer], preferred_element_type=jnp.float32)
        hidden = (hidden.astype(jnp.float32) + branch).astype(jnp.bfloat16)
    return hidden
```

```python
import jax
import jax.numpy as jnp
from jax import lax
from jax.sharding import PartitionSpec as P


class Places:
    def __init__(self):
        self.grp = lax.axis_size("grp")
        self.sp = lax.axis_size("sp")
        self.tp = lax.axis_size("tp")
        self.pairs = self.sp // 2
        self.hosts = [2 * i + 1 - i % 2 for i in range(self.pairs)]
        self.ends = [2 * i + i % 2 for i in range(self.pairs)]
        self.g = lax.axis_index("grp")
        self.s = lax.axis_index("sp")
        self.t = lax.axis_index("tp")
        self.pair = self.s // 2
        self.chips = self.tp // 2

    def host_of(self, pair):
        return 2 * pair + 1 - pair % 2

    def end_of(self, pair):
        return 2 * pair + pair % 2

    def is_host(self):
        return self.s == self.host_of(self.pair)

    def to_host(self, block):
        return lax.ppermute(block, "sp", list(zip(self.ends, self.hosts)))

    def to_end(self, block):
        return lax.ppermute(block, "sp", list(zip(self.hosts, self.ends)))

    def to_next_pair(self, block):
        route = [(2 * i + 1, self.hosts[i + 1]) for i in range(self.pairs - 1)]
        return lax.ppermute(block, "sp", route)

    def around_hosts(self, block, d):
        n = self.pairs
        return lax.ppermute(
            block, "sp", [(self.hosts[i], self.hosts[(i + d) % n]) for i in range(n)]
        )

    def around_grp(self, block, d):
        return lax.ppermute(block, "grp", [(i, (i + d) % self.grp) for i in range(self.grp)])

    def other_core(self, block):
        return lax.ppermute(block, "tp", [(i, i ^ 1) for i in range(self.tp)])

    def around_chips(self, block, d):
        return lax.ppermute(block, "tp", [(i, (i + 2 * d) % self.tp) for i in range(self.tp)])


def weight_pieces(at, weight):
    parts = at.grp
    unit = weight.shape[0] // parts

    def part(block, p):
        return lax.dynamic_slice_in_dim(block, p * unit, unit, 0)

    own_part = part(weight, at.g)
    end_first = at.to_host(own_part)
    end_rest = [at.to_host(part(weight, (at.g + d) % parts)) for d in range(1, parts)]
    end_of = at.end_of(at.pair)
    pieces = [(weight[p * unit : (p + 1) * unit], at.s * parts + p) for p in range(parts)]
    pieces.append((end_first, end_of * parts + at.g))
    for d in range(1, parts):
        pieces.append((end_rest[d - 1], end_of * parts + (at.g + d) % parts))
    for d in range(1, at.pairs):
        source = (at.pair + at.pairs - d) % at.pairs
        for block, shard in ((own_part, at.host_of(source)), (end_first, at.end_of(source))):
            here = at.around_hosts(block, d)
            pieces.append((here, shard * parts + at.g))
            for e in range(1, parts):
                there = at.around_grp(here, e)
                pieces.append((there, shard * parts + (at.g + parts - e) % parts))
    return pieces


class Gathered:
    def __init__(self, at, block, unit):
        self.at = at
        mine = [block] + [at.around_chips(block, d) for d in range(1, at.chips)]
        blocks = []
        for b in mine:
            blocks += [b, at.other_core(b)]
        self.blocks = blocks
        self.sub = block.shape[1] // unit
        self.units = jnp.stack(
            [b[:, j * unit : (j + 1) * unit] for b in blocks for j in range(self.sub)]
        )

    def unit(self, index):
        at = self.at
        source, j = index // self.sub, index % self.sub
        d = (at.t // 2 + at.chips - source // 2) % at.chips
        slot = 2 * d + jnp.where(source % 2 == at.t % 2, 0, 1)
        return lax.dynamic_index_in_dim(self.units, slot * self.sub + j, 0, keepdims=False)


def product(pieces, rows_of):
    total = None
    for weight, index in pieces:
        term = jnp.dot(rows_of(index), weight, preferred_element_type=jnp.float32)
        total = term if total is None else total + term
    return total


def shards(tokens, rms_gain, w_value, w_gate, taps, ln_gain, ln_bias, w_out):
    at = Places()
    layers = w_value.shape[0]
    features = rms_gain.shape[1]
    rows = tokens.shape[0]
    channels = w_out.shape[1] * at.sp
    reach = taps.shape[1]
    margin = -(-(reach - 1) // 16) * 16
    halo = layers * margin

    from_end = at.to_host(tokens)
    before = at.to_next_pair(tokens[rows - halo :])
    host_first = at.s % 2 == 0
    lower = jnp.where(host_first, tokens, from_end)
    upper = jnp.where(host_first, from_end, tokens)
    hidden = jnp.concatenate([before, lower, upper], axis=0)

    pieces = [
        (weight_pieces(at, w_value[l]), weight_pieces(at, w_gate[l]), weight_pieces(at, w_out[l]))
        for l in range(layers)
    ]
    in_unit = w_value.shape[1] // at.grp
    out_unit = w_out.shape[1] // at.grp
    for l in range(layers):
        value_pieces, gate_pieces, out_pieces = pieces[l]
        count = hidden.shape[0]
        whole = Gathered(at, hidden, min(in_unit, hidden.shape[1]))
        square = sum(
            jnp.sum(jnp.square(b.astype(jnp.float32)), axis=1, keepdims=True) for b in whole.blocks
        )
        scale = lax.rsqrt(square / features + 1e-06)
        gains = rms_gain[l].reshape(-1, 1, in_unit)

        def scaled(index):
            gain = lax.dynamic_index_in_dim(gains, index, 0, keepdims=False)
            return (whole.unit(index).astype(jnp.float32) * gain).astype(jnp.bfloat16)

        value = product(value_pieces, scaled) * scale
        gate = product(gate_pieces, scaled) * scale
        glu = (value * jax.nn.sigmoid(gate)).astype(jnp.bfloat16)
        left = halo - l * margin
        is_real = (at.pair > 0) | (lax.broadcasted_iota(jnp.int32, (count, 1), 0) >= left)
        extended = jnp.where(is_real, glu, jnp.zeros_like(glu)).astype(jnp.float32)
        out_rows = count - margin
        first = margin - (reach - 1)
        conv = jnp.zeros((out_rows, extended.shape[1]), jnp.float32)
        for k in range(reach):
            conv = conv + taps[l, k][None, :] * extended[first + k : first + k + out_rows]
        sums = jnp.stack([jnp.sum(conv, axis=1), jnp.sum(conv * conv, axis=1)])
        sums = jnp.sum(lax.all_gather(sums, "tp"), axis=0)
        mean = sums[0][:, None] / channels
        var = sums[1][:, None] / channels - mean * mean
        shaped = (conv - mean) * lax.rsqrt(var + 1e-05) * ln_gain[l][None, :] + ln_bias[l][None, :]
        act = jax.nn.silu(shaped).astype(jnp.bfloat16)
        acts = Gathered(at, act, min(out_unit, act.shape[1]))
        branch = product(out_pieces, acts.unit)
        hidden = (hidden[margin:].astype(jnp.float32) + branch).astype(jnp.bfloat16)
    low, high = hidden[:rows], hidden[rows:]
    back = at.to_end(jnp.where(host_first, high, low))
    mine = jnp.where(host_first, low, high)
    return jnp.where(at.is_host(), mine, back)


def solution(mesh):
    return jax.shard_map(
        shards,
        mesh=mesh,
        in_specs=(
            P(("grp", "sp"), "tp"),
            P(),
            P(None, "sp", "tp"),
            P(None, "sp", "tp"),
            P(None, None, "tp"),
            P(None, "tp"),
            P(None, "tp"),
            P(None, "sp", "tp"),
        ),
        out_specs=P(("grp", "sp"), "tp"),
        check_vma=False,
    )
```
